32 devices in a mesh: sp: 8 (over z, y), dp: 4 (over x, core).
Axes of the slice: x: 2, y: 2, z: 4, core: 2. Of those that a mesh axis runs over, the one named last changes fastest.
Arguments:
- u_pre: bfloat16 [4, 8192, 2048], P('dp', 'sp'), may hold values from -6 to 6
- v_pre: bfloat16 [4, 8192, 2048], P('dp', 'sp'), may hold values from -6 to 6
- d_out: bfloat16 [4, 8192, 2048], P('dp', 'sp'), may hold values from -6 to 6
- w_mix: bfloat16 [16, 128, 128], replicated, may hold values from -0.5 to 0.5
- mix_bias: float32 [16, 128], replicated, may hold values from 0.1 to 1.9
- norm_gain: float32 [16, 128], replicated, may hold values from 0.1 to 1.9
- norm_shift: float32 [16, 128], replicated, may hold values from -3 to 3
- w_out: bfloat16 [2048, 2048], P('dp'), may hold values from -0.125 to 0.125
Outputs:
- grad_u: bfloat16 [4, 8192, 2048], P('dp', 'sp')
- grad_v: bfloat16 [4, 8192, 2048], P('dp', 'sp')
- grad_w_out: float32 [2048, 2048], P('dp')
- grad_w_mix: float32 [16, 128, 128], replicated
- grad_mix_bias: float32 [16, 128], replicated
- grad_gain: float32 [16, 128], replicated
- grad_shift: float32 [16, 128], replicated
The draws below stay inside these ranges and needn't reach their ends.
All inputs are finite; a program needn't handle non-finite values.
Results may differ from the reference program's by a relative error of at most 0.012.
Values may be sent and summed in bfloat16 or wider, within the bound.
A program may use at most 192 MiB of HBM per device.

```python
import jax
import jax.numpy as jnp
from jax import lax

D = 2048
GROUPS = 16
CHANS = 128
BLOCK = 128
SGU_W = 2048
SEQLEN = 8192
SEQS = 4


def block_scale(stream_key, extent, shards, least, largest):
    def one(axis_at, blocks):
        heights = jax.random.uniform(jax.random.fold_in(jax.random.fold_in(stream_key, 6), axis_at), (blocks,), jnp.float32, least / len(shards), largest / len(shards))
        return jnp.repeat(jnp.exp(heights), extent[axis_at] // blocks).reshape((-1,) + (1,) * (len(extent) - axis_at - 1))

    factor_of = one(*shards[0])
    for cut in shards[1:]:
        factor_of = factor_of * one(*cut)
    return factor_of


def scatter_about(stream_key, shape, spread, bound, split=(), kind=jnp.bfloat16):
    entries = jax.random.normal(stream_key, shape, jnp.float32) * spread
    if len(split) > 0:
        entries = block_scale(stream_key, shape, split, -0.22, 0.18) * entries
    return jnp.clip(entries, min=-bound, max=bound).astype(kind)


def setup_inputs(seed: int = 0) -> dict:
    arg_keys = jax.random.split(jax.random.key(seed), 9)
    u_pre = scatter_about(arg_keys[0], (SEQS, SEQLEN, SGU_W), 1.0, 6.0, ((0, 4), (1, 8)))
    v_pre = scatter_about(arg_keys[1], (SEQS, SEQLEN, SGU_W), 1.0, 6.0, ((0, 4), (1, 8)))
    d_out = scatter_about(arg_keys[2], (SEQS, SEQLEN, D), 1.0, 6.0, ((0, 4), (1, 8)))
    w_mix = scatter_about(arg_keys[3], (GROUPS, BLOCK, BLOCK), BLOCK ** -0.5, 0.5)
    mix_bias = jnp.clip(1.0 + 0.18 * jax.random.normal(arg_keys[4], (GROUPS, BLOCK), jnp.float32), 0.1, 1.9)
    norm_gain = jnp.clip(1.0 + 0.18 * jax.random.normal(arg_keys[5], (GROUPS, CHANS), jnp.float32), 0.1, 1.9)
    norm_shift = scatter_about(arg_keys[6], (GROUPS, CHANS), 0.5, 3.0, (), jnp.float32)
    w_out = scatter_about(arg_keys[7], (SGU_W, D), SGU_W ** -0.5, 0.125, ((0, 4),))
    return {"u_pre": u_pre, "v_pre": v_pre, "d_out": d_out, "w_mix": w_mix, "mix_bias": mix_bias, "norm_gain": norm_gain, "norm_shift": norm_shift, "w_out": w_out}


EPS = 1e-05

def mechanism(grad_s, u_pre, v_pre, w_mix, mix_bias, gain, shift):
    items, length, width = grad_s.shape
    groups, span = (w_mix.shape[0], w_mix.shape[1])
    chans = width // groups
    shape = (items, length // span, span, groups, chans)
    u_val = u_pre.astype(jnp.float32).reshape(shape)
    v_val = v_pre.astype(jnp.float32).reshape(shape)
    cotan = grad_s.astype(jnp.float32).reshape(shape)
    upper, u_back = jax.vjp(jax.nn.gelu, u_val)
    gated, v_back = jax.vjp(jax.nn.gelu, v_val)
    centre = gated - lax.optimization_barrier(jnp.mean(gated, axis=-1, keepdims=True))
    inverse = lax.rsqrt(lax.optimization_barrier(jnp.mean(centre * centre, axis=-1, keepdims=True)) + EPS)
    scaled = centre * inverse
    normed = (scaled * gain + shift).astype(jnp.bfloat16)
    lower = jnp.tril(jnp.ones((span, span), dtype=bool))
    w_low = jnp.where(lower[None], w_mix, jnp.zeros_like(w_mix))
    mixed = jnp.einsum('gts,insgc->intgc', w_low.astype(jnp.float32), normed.astype(jnp.float32))
    mixed = mixed + jnp.transpose(mix_bias)[:, :, None]
    gated_out = (upper * mixed).astype(jnp.bfloat16)
    d_mixed = cotan * upper
    d_mixed_b = d_mixed.astype(jnp.bfloat16)
    grad_u = u_back(cotan * mixed)[0].astype(jnp.bfloat16).reshape(items, length, width)
    grad_bias = jnp.transpose(lax.optimization_barrier(jnp.sum(d_mixed, axis=(0, 1, 4))))
    grad_w = jnp.einsum('intgc,insgc->gts', d_mixed_b.astype(jnp.float32), normed.astype(jnp.float32))
    grad_w = jnp.where(lower[None], grad_w, jnp.zeros_like(grad_w))
    d_normed = jnp.einsum('gts,intgc->insgc', w_low.astype(jnp.float32), d_mixed_b.astype(jnp.float32))
    grad_gain = lax.optimization_barrier(jnp.sum(d_normed * scaled, axis=(0, 1, 2)))
    grad_shift = lax.optimization_barrier(jnp.sum(d_normed, axis=(0, 1, 2)))
    d_scaled = d_normed * gain
    d_gated = inverse * (d_scaled - lax.optimization_barrier(jnp.mean(d_scaled, axis=-1, keepdims=True)) - scaled * lax.optimization_barrier(jnp.mean(d_scaled * scaled, axis=-1, keepdims=True)))
    grad_v = v_back(d_gated)[0].astype(jnp.bfloat16).reshape(items, length, width)
    return (grad_u, grad_v, gated_out.reshape(items, length, width), grad_w, grad_bias, grad_gain, grad_shift)

def reference(u_pre, v_pre, d_out, w_mix, mix_bias, norm_gain, norm_shift, w_out):
    flat_d = d_out.reshape(-1, D)
    grad_s = jnp.dot(flat_d, jnp.transpose(w_out), preferred_element_type=jnp.float32)
    grad_s = grad_s.astype(jnp.bfloat16).reshape(SEQS, SEQLEN, SGU_W)

    def one_sequence(packed):
        cot, upre, vpre = packed
        return mechanism(cot[None], upre[None], vpre[None], w_mix, mix_bias, norm_gain, norm_shift)
    grad_u, grad_v, gated_out, grad_w, grad_bias, grad_gain, grad_shift = lax.map(one_sequence, (grad_s, u_pre, v_pre))
    grad_u = grad_u.reshape(SEQS, SEQLEN, SGU_W)
    grad_v = grad_v.reshape(SEQS, SEQLEN, SGU_W)
    flat_s = gated_out.reshape(-1, SGU_W)
    grad_w_out = jnp.dot(jnp.transpose(flat_s), flat_d, preferred_element_type=jnp.float32)
    return (grad_u, grad_v, grad_w_out, lax.optimization_barrier(jnp.sum(grad_w, axis=0)), lax.optimization_barrier(jnp.sum(grad_bias, axis=0)), lax.optimization_barrier(jnp.sum(grad_gain, axis=0)), lax.optimization_barrier(jnp.sum(grad_shift, axis=0)))
```

```python
import functools

import jax
import jax.numpy as jnp
from jax import lax
from jax.experimental import pallas as pl
from jax.experimental.pallas import tpu as pltpu
from jax.sharding import PartitionSpec as P

EPS = 1e-05
K0 = 0.7978845608028654
K1 = 0.044715
F32 = jnp.float32
BF16 = jnp.bfloat16


TIMES = (6.0, 2.4, 27.7, 2.05, 6, 2.5)
T_W = (13.5, 19.5, 21.6, 27.0)
T_WZ = ((0, 2), (3, 5))
T_UNIT = (
    (25.0, 33.5, 39.5, 46.0, 52.0, 58.0, 78.2),
    (37.0, 46.2, 52.0, 58.2, 64.6, 70.0, 78.4),
    (48.0, 56.6, 65.0, 73.0, 81.5),
    (56.5, 62.8, 68.5, 74.0, 81.0),
    (64.0, 69.5, 75.0, 80.5, 86.0),
)
T_END = (65.2, 62.9, 71.5, 69.0, 76.5)


def gelu_parts(a):
    sq = a * a
    t = jnp.tanh(a * (K0 + (K0 * K1) * sq))
    half = 0.5 * (1.0 + t)
    return sq, t, half


def gelu(a):
    _, _, half = gelu_parts(a)
    return a * half


def gelu_both(a):
    sq, t, half = gelu_parts(a)
    slope = half + (0.5 * a) * (1.0 - t * t) * (K0 + (3.0 * K0 * K1) * sq)
    return a * half, slope


def norm_parts(gated):
    centre = gated - jnp.mean(gated, axis=-1, keepdims=True)
    inverse = lax.rsqrt(jnp.mean(centre * centre, axis=-1, keepdims=True) + EPS)
    return centre * inverse, inverse


def mm(a, b, ca, cb):
    return lax.dot_general(a, b, (((ca,), (cb,)), ((), ())), preferred_element_type=F32)


def each(lo, hi, fn):
    def body(i, carry):
        fn(i)
        return carry
    lax.fori_loop(lo, hi, body, 0)


def kernel(
    dims,
    u_hbm, v_hbm, d_hbm, wmix_hbm, bias_hbm, gain_hbm, shift_hbm, w_hbm,
    gu_ref, gv_ref, dw_ref, sm_ref,
    u_ref, v_ref, d_ref, wmix_ref, bias_row, gain_ref, shift_ref, bias_ref, u_s, v_s, in_s,
    wfull, part, rcore, rx, ry, rz, ag, gs, got, wl_ref, wlt_ref, acc,
    sbuf, acore, srecv, fin,
    wown_s, wown_r, wx_s, wx_r, wy_s, wy_r, wz_s, wz_r, wfw_s, wfw_r,
    core_s, core_r, xs_s, xs_r, yr_s, yr_r, zr_s, zr_r, za_s, za_r, ya_s, ya_r,
    sa_s, sa_r, sb_s, sb_r, sc_s, sc_r, sd_s, sd_r,
):
    n_y, n_z, n_dp, gpc, span, chans, width, rows, prow, n_own = dims
    n_sp = n_y * n_z
    pairs = n_dp // 2
    n_chips = n_sp * pairs
    nb = rows // span
    s = lax.axis_index("sp")
    dpi = lax.axis_index("dp")
    x = dpi // 2
    c = dpi % 2
    y = s % n_y
    z = s // n_y
    zp = z % 2
    other = 1 - c
    mate = {"sp": s, "dp": 2 * x + other}
    chip = s * pairs + x

    def rc(src, dst, ssem, rsem, dev):
        return pltpu.make_async_remote_copy(
            src_ref=src, dst_ref=dst, send_sem=ssem, recv_sem=rsem,
            device_id=dev, device_id_type=pl.DeviceIdType.MESH,
        )

    def up(k):
        return (x + k) % pairs

    def down(k):
        return (x + pairs - k) % pairs

    def at_x(k):
        return {"sp": s, "dp": 2 * up(k) + c}

    def at_y(o):
        return {"sp": z * n_y + (y + o) % n_y, "dp": dpi}

    def at_z(o):
        return {"sp": (z + o) % n_z * n_y + y, "dp": dpi}

    def at_chip(o):
        to = (chip + o) % n_chips
        return {"sp": to // pairs, "dp": 2 * (to % pairs) + c}

    def w_own():
        return rc(wfull.at[dpi], wfull.at[dpi], wown_s, wown_r, mate)

    def w_x(k, h):
        block = wfull.at[dpi, y, zp, h]
        return rc(block, block, wx_s.at[k, h], wx_r.at[k, h], at_x(k))

    def w_y(k, h, o):
        block = wfull.at[2 * down(k) + c, y, zp, h]
        return rc(block, block, wy_s.at[k, h, o], wy_r.at[k, h, o], at_y(o))

    def w_z(k, h, o):
        a = (y + o) % n_y
        block = wfull.at[2 * down(k) + c, a, zp, h]
        to = {"sp": (z + 1 - 2 * zp) * n_y + y, "dp": dpi}
        return rc(block, block, wz_s.at[k, h, o], wz_r.at[k, h, o], to)

    def w_fw(k, a, zz, h):
        block = wfull.at[2 * down(k) + c, a, zz, h]
        return rc(block, block, wfw_s.at[k, a, zz, h], wfw_r.at[k, a, zz, h], mate)

    units = [(q, 0, span) for q in range(gpc - 1)]
    units += [(gpc - 1, 0, span // 2), (gpc - 1, span // 2, span // 2)]
    half_z = n_z // 2

    def gid(xx, cc, q):
        return (2 * xx + cc) * gpc + q

    def t_core(k, q):
        return rc(part.at[gid(up(k), other, q)], rcore.at[k, q], core_s.at[k, q], core_r.at[k, q], mate)

    def t_x(k, n, a):
        q, lo, size = units[n]
        at = pl.ds(lo, size)
        return rc(
            part.at[gid(up(k), c, q), a, :, at], rx.at[k - 1, q, a, :, at],
            xs_s.at[k, n, a], xs_r.at[k, n, a], at_x(k),
        )

    def t_yr(n, o, b):
        q, lo, size = units[n]
        at = pl.ds(lo, size)
        return rc(
            part.at[gid(x, c, q), (y + o) % n_y, b, at], ry.at[q, o - 1, b, at],
            yr_s.at[n, o], yr_r.at[n, o, b], at_y(o),
        )

    def all_yr(n, o):
        q, lo, size = units[n]
        block = part.at[gid(x, c, q), (y + o) % n_y, :, pl.ds(lo, size)]
        return rc(block, block, yr_s.at[n, o], yr_r.at[n, o, 0], mate)

    def z_send(n, b, slot, dst_slot, to):
        q, lo, size = units[n]
        at = pl.ds(lo, size)
        return rc(
            part.at[gid(x, c, q), y, b, at], rz.at[q, dst_slot, at],
            zr_s.at[n, slot], zr_r.at[n, slot], to,
        )

    to_pair = {"sp": (z + 1 - 2 * zp) * n_y + y, "dp": dpi}
    pair_z = z + 1 - 2 * zp

    def t_zr(n, o):
        return z_send(n, (z + o) % n_z, o, o - 1, at_z(o))

    def t_zp(n, m):
        return z_send(n, (pair_z + 2 * m) % n_z, 2 * m + 1, m, to_pair)

    def t_zc(n, m):
        return z_send(n, (z + 2 * m) % n_z, 2 * m, half_z + m - 1, at_z(2 * m))

    def gathered(n, b, ssem, rsem, to):
        q, lo, size = units[n]
        block = ag.at[q, y, b, pl.ds(lo, size)]
        return rc(block, block, ssem, rsem, to)

    def t_za(n, o):
        return gathered(n, z, za_s.at[n, o], za_r.at[n, o], at_z(o))

    def t_ap(n, m):
        return gathered(n, (z + 2 * m) % n_z, za_s.at[n, 2 * m + 1], za_r.at[n, 2 * m + 1], to_pair)

    def t_ya(n, o, b):
        return gathered(n, b, ya_s.at[n, o], ya_r.at[n, o], at_y(o))

    def all_ya(n, o):
        q, lo, size = units[n]
        block = ag.at[q, y, :, pl.ds(lo, size)]
        return rc(block, block, ya_s.at[n, o], ya_r.at[n, o], mate)

    def t_sa(k, j):
        chunk = 2 * down(k) + j
        return rc(sbuf.at[chunk, other], acore.at[chunk], sa_s.at[chunk], sa_r.at[chunk], mate)

    def t_sb(chunk, o):
        to = (chip + o) % n_chips
        return rc(sbuf.at[chunk, c, to % n_own], srecv.at[chunk, o - 1], sb_s.at[chunk], sb_r.at[chunk], at_chip(o))

    def t_sc(j, o):
        block = fin.at[j, c, chip % n_own]
        return rc(block, block, sc_s.at[j], sc_r.at[j], at_chip(o))

    def all_sb(chunk):
        return rc(srecv.at[chunk], srecv.at[chunk], sb_s.at[chunk], sb_r.at[chunk], mate)

    def all_sc(j):
        block = fin.at[j, c, pl.ds(0, n_own - 1)]
        return rc(block, block, sc_s.at[j], sc_r.at[j], mate)

    def t_sd(j):
        return rc(fin.at[j, c], fin.at[j, c], sd_s.at[j], sd_r.at[j], mate)

    def owner(t, fn):
        if n_own == n_chips:
            fn()
        else:
            pl.when(t < n_own)(fn)

    row = lax.broadcasted_iota(jnp.int32, (span, span), 0)
    col = lax.broadcasted_iota(jnp.int32, (span, span), 1)
    lower = row >= col
    share = 2 * gpc * chans

    def cols(k):
        return pl.ds(pl.multiple_of(up(k) * share, share), share)

    small = [
        pltpu.make_async_copy(src, dst, in_s.at[n])
        for n, (src, dst) in enumerate((
            (bias_hbm, bias_row), (gain_hbm, gain_ref), (shift_hbm, shift_ref), (wmix_hbm, wmix_ref),
        ))
    ]
    near = {k: (
        pltpu.make_async_copy(v_hbm.at[:, cols(k)], v_ref.at[:, cols(k)], v_s.at[k]),
        pltpu.make_async_copy(u_hbm.at[:, cols(k)], u_ref.at[:, cols(k)], u_s.at[k]),
    ) for k in range(pairs)}
    first_k = 1 % pairs
    load_w = pltpu.make_async_copy(w_hbm, wfull.at[dpi], in_s.at[4])
    load_d = pltpu.make_async_copy(d_hbm, d_ref, in_s.at[5])
    for load in small:
        load.start()
    for load in near[first_k]:
        load.start()
    load_w.start()
    load_d.start()
    for k in range(pairs):
        if k != first_k:
            for load in near[k]:
                load.start()
    barrier = pltpu.get_barrier_semaphore()
    pl.semaphore_signal(barrier, inc=1, device_id=mate, device_id_type=pl.DeviceIdType.MESH)
    each(1, n_chips, lambda o: pl.semaphore_signal(
        barrier, inc=1, device_id=at_chip(o), device_id_type=pl.DeviceIdType.MESH,
    ))

    def lanes(g):
        return pl.ds(pl.multiple_of(g * chans, chans), chans)

    def far_group(i, h):
        return gid(up((i // gpc + 1) % pairs), (c + h) % 2, i % gpc)

    def low_weights(g, h):
        wl_ref[h] = jnp.where(lower, wmix_ref[g], jnp.zeros((), BF16))

    def forward_block(i, b):
        at = pl.ds(pl.multiple_of(b * span, span), span)
        for h in range(2):
            g = far_group(i, h)
            scaled, _ = norm_parts(gelu(v_ref[at, lanes(g)].astype(F32)))
            normed = (scaled * gain_ref[g] + shift_ref[g]).astype(BF16)
            mixed = mm(wl_ref[h], normed, 1, 0) + bias_ref[g]
            out = (gelu(u_ref[at, lanes(g)].astype(F32)) * mixed).astype(BF16)
            got[i % 2, h * span : (h + 1) * span, at] = out.T

    def core_sum(k, q):
        t_core(k, q).wait_recv()
        g = gid(up(k), c, q)

        def one(j):
            a, b = j // n_z, j % n_z
            part[g, a, b] = (part[g, a, b].astype(F32) + rcore[k, q, a, b].astype(F32)).astype(BF16)
        each(0, n_sp, one)

    def x_start(k, n):
        for o in range(n_y):
            t_x(k, n, (y + 1 + o) % n_y).start()

    per_block = n_sp // nb

    def product_block(i, b):
        keep = far_group(i, 0)
        give = far_group(i, 1)
        wide = per_block * width
        r = mm(got[i % 2], d_ref[:, pl.ds(pl.multiple_of(b * wide, wide), wide)], 1, 0)
        for e in range(per_block):
            j = b * per_block + e
            at = slice(e * width, (e + 1) * width)
            part[keep, j // n_z, j % n_z] = r[:span, at].astype(BF16)
            part[give, j // n_z, j % n_z] = r[span:, at].astype(BF16)

    def give_core(i):
        t_core((i // gpc + 1) % pairs, i % gpc).start()

    def w_from_x(h):
        for k in range(1, pairs):
            w_x(k, h).wait_recv()
            for o in range(1, n_y):
                w_y(k, h, o).start()
            w_z(k, h, 0).start()
            w_fw(k, y, zp, h).start()

    def w_from_y(h):
        for k in range(1, pairs):
            for o in range(1, n_y):
                w_y(k, h, o).wait_recv()
            for o in range(1, n_y):
                w_z(k, h, o).start()
                w_fw(k, (y + o) % n_y, zp, h).start()

    def w_from_z(h, o):
        for k in range(1, pairs):
            w_z(k, h, o).wait_recv()
            w_fw(k, (y + o) % n_y, 1 - zp, h).start()

    def w_ready(k):
        for h in range(2):
            for zz in range(2):
                for a in range(n_y):
                    w_fw(k, a, zz, h).wait_recv()

    def yr_start(n):
        q, lo, size = units[n]
        if lo == 0:
            t_core(0, q).wait_recv()
        at = pl.ds(lo, size)
        g = gid(x, c, q)
        for o in range(1, n_y):
            a = (y + o) % n_y
            for k in range(1, pairs):
                t_x(k, n, a).wait_recv()

            def one(b):
                total = part[g, a, b, at].astype(F32) + rcore[0, q, a, b, at].astype(F32)
                for k in range(1, pairs):
                    total = total + rx[k - 1, q, a, b, at].astype(F32)
                part[g, a, b, at] = total.astype(BF16)
                t_yr(n, o, b).start()
            each(1, n_z + 1, lambda j: one((z + j) % n_z))

    def own_total(n, b):
        q, lo, size = units[n]
        at = pl.ds(lo, size)
        total = part[gid(x, c, q), y, b, at].astype(F32) + rcore[0, q, y, b, at].astype(F32)
        for k in range(1, pairs):
            total = total + rx[k - 1, q, y, b, at].astype(F32)
        for o in range(1, n_y):
            total = total + ry[q, o - 1, b, at].astype(F32)
        return total

    def own_ready(n):
        for k in range(1, pairs):
            t_x(k, n, y).wait_recv()

    def y_ready(n, b):
        for o in range(1, n_y):
            t_yr(n, o, b).wait_recv()

    def keep_sum(n, b, total):
        q, lo, size = units[n]
        part[gid(x, c, q), y, b, pl.ds(lo, size)] = total.astype(BF16)

    def from_z(n, slot):
        q, lo, size = units[n]
        return rz[q, slot, pl.ds(lo, size)].astype(F32)

    def whole(n, total):
        q, lo, size = units[n]
        ag[q, y, z, pl.ds(lo, size)] = total.astype(BF16)
        for o in range(1, n_y):
            t_ya(n, o, z).start()

    def zr_start(n):
        own_ready(n)
        for j in range(1, n_z):
            b = (z + j) % n_z
            y_ready(n, b)
            keep_sum(n, b, own_total(n, b))
            t_zr(n, j).start()

    def za_start(n):
        y_ready(n, z)
        total = own_total(n, z)
        for o in range(1, n_z):
            t_zr(n, o).wait_recv()
            total = total + from_z(n, o - 1)
        whole(n, total)
        for o in range(1, n_z):
            t_za(n, o).start()

    def ya_start(n):
        for o in range(1, n_z):
            t_za(n, o).wait_recv()
            for a in range(1, n_y):
                t_ya(n, a, (z + n_z - o) % n_z).start()

    def zp_start(n):
        own_ready(n)
        for j in range(half_z):
            m = half_z - 1 - j
            b = (pair_z + 2 * m) % n_z
            y_ready(n, b)
            keep_sum(n, b, own_total(n, b))
            t_zp(n, m).start()

    def zc_start(n):
        for m in range(1, half_z):
            b = (z + 2 * m) % n_z
            y_ready(n, b)
            t_zp(n, m).wait_recv()
            keep_sum(n, b, own_total(n, b) + from_z(n, m))
            t_zc(n, m).start()

    def ac_start(n):
        y_ready(n, z)
        t_zp(n, 0).wait_recv()
        total = own_total(n, z) + from_z(n, 0)
        for m in range(1, half_z):
            t_zc(n, m).wait_recv()
            total = total + from_z(n, half_z + m - 1)
        whole(n, total)
        for m in range(1, half_z):
            t_za(n, 2 * m).start()
        t_ap(n, 0).start()

    def ap_start(n):
        for m in range(1, half_z):
            t_za(n, 2 * m).wait_recv()
            t_ap(n, half_z - m).start()
            for a in range(1, n_y):
                t_ya(n, a, (z + n_z - 2 * m) % n_z).start()

    def yb_start(n):
        for m in range(half_z):
            t_ap(n, m).wait_recv()
            for a in range(1, n_y):
                t_ya(n, a, (pair_z + 2 * m) % n_z).start()

    def dw_done(n):
        q, lo, size = units[n]
        for o in range(1, n_y):
            all_ya(n, o).wait_recv()

        def one(j):
            dw_ref[q, j, pl.ds(lo, size)] = ag[q, j // n_z, j % n_z, pl.ds(lo, size)]
        each(0, n_sp, one)

    def bias_column(g):
        bias_ref[g] = jnp.broadcast_to(bias_row[g], (span, span)).T

    for load in small:
        load.wait()
    each(0, n_dp * gpc, lambda g: bias_column(g))
    for load in near[first_k]:
        load.wait()
    for h in range(2):
        low_weights(far_group(0, h), h)

    def first_blocks(b):
        for n in range(4):
            forward_block(0, 4 * b + n)
    each(0, nb // 4, first_blocks)
    load_w.wait()
    pl.semaphore_wait(barrier, n_chips)
    for h in range(2):
        for k in range(1, pairs):
            w_x(k, h).start()
    w_own().start()
    load_d.wait()
    for k in range(pairs):
        if k != first_k:
            for load in near[k]:
                load.wait()

    n_far = (pairs - 1) * gpc
    n_fwd = pairs * gpc
    per_chunk = gpc // 2
    n_steps = n_dp * per_chunk
    n_slots = 2 * n_steps
    before = {}
    after = {}
    late = []

    def run(todo):
        for fn, args in todo:
            fn(*args)

    def sa_start(k, j):
        t_sa(k, j).start()

    def sb_start(k, j):
        t_sa(k, j).wait_recv()
        chunk = 2 * down(k) + j

        def one(p):
            sbuf[chunk, c, p] = (sbuf[chunk, c, p].astype(F32) + acore[chunk, p].astype(F32)).astype(BF16)
        each(0, n_own, one)
        each(1, n_chips, lambda o: owner((chip + o) % n_chips, lambda: t_sb(chunk, o).start()))

    def sc_start(j):
        def mine():
            for xx in range(pairs):
                chunk = 2 * xx + j
                all_sb(chunk).wait_recv()
                total = lax.fori_loop(
                    1, n_chips, lambda o, a: a + srecv[chunk, o - 1].astype(F32),
                    sbuf[chunk, c, chip % n_own].astype(F32),
                )
                fin[j, c, chip % n_own, xx] = total.astype(BF16)
            each(1, n_chips, lambda o: t_sc(j, o).start())
        owner(chip, mine)

    def sd_start(j):
        if n_own == n_chips:
            all_sc(j).wait_recv()
        else:
            each(1, n_chips, lambda o: owner((chip + n_chips - o) % n_chips, lambda: t_sc(j, o).wait_recv()))
        t_sd(j).start()

    fwd_0, fwd_us, bwd_0, bwd_us, pause_at, pause_us = TIMES

    def put(time, fn, *args):
        step = 0
        while step <= n_fwd and fwd_0 + fwd_us * step < time:
            step += 1
        at_slot = 0
        while at_slot < n_slots and bwd_0 + bwd_us * (at_slot + 1) + pause_us * (at_slot >= pause_at) < time:
            at_slot += 1
        if step <= n_fwd:
            before.setdefault(max(step, 1), []).append((time, fn, args))
        elif at_slot < n_slots:
            after.setdefault(at_slot, []).append((time, fn, args))
        else:
            late.append((time, fn, args))

    def put_slot(at_slot, time, fn, *args):
        if at_slot < n_slots:
            after.setdefault(at_slot, []).append((time, fn, args))
        else:
            late.append((time, fn, args))

    def in_order(todo):
        return [(fn, args) for _, fn, args in sorted(todo, key=lambda item: item[0])]

    put(T_W[0], w_from_x, 0)
    put(T_W[1], w_from_x, 1)
    put(T_W[2], w_from_y, 0)
    put(T_W[3], w_from_y, 1)
    need = 4 * per_chunk - 3
    for h in range(2):
        for o in range(n_y):
            put_slot(min(need, T_WZ[min(o, 1)][h]), 0.0 + o + h / 2, w_from_z, h, o)
    pair_stages = (yr_start, zp_start, zc_start, ac_start, ap_start, yb_start, dw_done)
    line_stages = (yr_start, zr_start, za_start, ya_start, dw_done)
    for n in range(len(units)):
        when = T_UNIT[n + 5 - len(units)]
        stages = line_stages if len(when) == 5 else pair_stages
        for fn, time in zip(stages, when):
            put(time, fn, n)
    for turn in range(n_dp):
        end = 2 * (turn + 1) * per_chunk
        put_slot(end - 1, 0.0, sa_start, turn // 2, turn % 2)
        put_slot(end, 0.5 if end < n_slots else T_END[0], sb_start, turn // 2, turn % 2)
    put(T_END[1], sc_start, 0)
    put(T_END[2], sc_start, 1)
    put(T_END[3], sd_start, 0)
    put(T_END[4], sd_start, 1)

    def sd_done():
        for j in range(2):
            t_sd(j).wait_recv()
    put(1000.0, sd_done)

    def core_sums(last):
        @pl.when((last >= 0) & (last < n_far))
        def _():
            k = (last // gpc + 1) % pairs
            core_sum(k, last % gpc)
            for kk in range(1, pairs):
                for n, unit in enumerate(units):
                    @pl.when(last == (kk - 1) * gpc + unit[0])
                    def _(kk=kk, n=n):
                        x_start(kk, n)

    def forward_step(i):
        for h in range(2):
            low_weights(far_group(i, h), h)

        def one(b):
            for n in range(4):
                product_block(i - 1, 4 * b + n)
            for n in range(4):
                forward_block(i, 4 * b + n)
        each(0, nb // 4, one)
        give_core(i - 1)
        core_sums(i - 2)
        for step in sorted(before):
            @pl.when(i == step)
            def _(step=step):
                run(in_order(before[step]))

    each(1, n_fwd, forward_step)
    each(0, nb, lambda b: product_block(n_fwd - 1, b))
    give_core(n_fwd - 1)
    core_sums(n_fwd - 2)
    core_sums(n_fwd - 1)
    w_own().wait_recv()
    run(in_order(before.get(n_fwd, [])))

    def backward_block(i, p):
        chunk, two = place(i)
        first = chunk * gpc + 2 * two
        for h in range(2):
            g = first + h
            gain = gain_ref[g]
            for e in range(2):
                at = pl.ds(pl.multiple_of((2 * p + e) * span, span), span)
                gated, v_slope = gelu_both(v_ref[at, lanes(g)].astype(F32))
                scaled, inverse = norm_parts(gated)
                normed = (scaled * gain + shift_ref[g]).astype(BF16)
                mixed = mm(wl_ref[h], normed, 1, 0) + bias_ref[g]
                upper, u_slope = gelu_both(u_ref[at, lanes(g)].astype(F32))
                cot = gs[i % 2, at, h * chans : (h + 1) * chans].astype(F32)
                dm = cot * upper
                dmb = dm.astype(BF16)
                gu_ref[at, lanes(g)] = (cot * mixed * u_slope).astype(BF16)
                acc[h, 0] += dm
                acc[h, 1] += mm(dmb, normed, 1, 1)
                dn = mm(wlt_ref[h], dmb, 1, 0)
                acc[h, 2] += dn * scaled
                acc[h, 3] += dn
                e_ = dn * gain
                m1 = jnp.mean(e_, axis=-1, keepdims=True)
                m2 = jnp.mean(e_ * scaled, axis=-1, keepdims=True)
                gv_ref[at, lanes(g)] = (v_slope * (inverse * (e_ - m1 - scaled * m2))).astype(BF16)

    def group_sums(h, chunk, q):
        grad_w = jnp.where(lower, acc[h, 1], 0.0)
        g_bias = jnp.sum(acc[h, 0].T, axis=0, keepdims=True)
        g_gain = jnp.sum(acc[h, 2], axis=0, keepdims=True)
        g_shift = jnp.sum(acc[h, 3], axis=0, keepdims=True)
        r16 = lax.broadcasted_iota(jnp.int32, (16, chans), 0)
        c16 = lax.broadcasted_iota(jnp.int32, (16, chans), 1)
        extra = jnp.where(r16 % 3 == 0, g_bias, jnp.where(r16 % 3 == 1, g_gain, g_shift))
        turned = pltpu.roll(extra, chans // 2, 1)
        top = jnp.where(c16 < chans // 2, grad_w[:16], jnp.where(r16 < 3, turned, jnp.where(r16 < 6, extra, 0.0)))
        per = span // prow
        hq = gpc // 2
        first = q % hq * per
        for p in range(per):
            block = grad_w[p * prow : (p + 1) * prow]
            if p == 0:
                block = jnp.concatenate([top, block[16:]], axis=0) if prow > 16 else top
            sbuf[chunk, q // hq, first + p] = block.astype(BF16)

    flat = wfull.reshape(n_dp, wfull.shape[1] * wfull.shape[2] * wfull.shape[3] * wfull.shape[4], wfull.shape[5])

    def place(i):
        turn = i // per_chunk
        return 2 * down(turn // 2) + turn % 2, i % per_chunk

    def cotangent_block(i, p):
        chunk, two = place(i)
        at = pl.ds(pl.multiple_of(p * 2 * span, 2 * span), 2 * span)
        these = pl.ds(pl.multiple_of(two * 2 * span, 2 * span), 2 * span)
        gs[i % 2, at, :] = mm(d_ref[at, :], flat[chunk, these, :], 1, 1).astype(BF16)

    n_pairs = nb // 2
    each(0, n_pairs, lambda p: cotangent_block(0, p))

    def slot(t):
        i = t // 2
        chunk, two = place(i)

        @pl.when(t % 2 == 0)
        def _():
            for k in range(1, pairs):
                @pl.when(i + 1 == 2 * k * per_chunk)
                def _(k=k):
                    w_ready(k)
            acc[...] = jnp.zeros_like(acc)
            for h in range(2):
                low_weights(chunk * gpc + 2 * two + h, h)
                wlt_ref[h] = wl_ref[h].T

        def one(p):
            for u in range(2):
                cotangent_block((i + 1) % n_steps, 2 * p + u)
            for u in range(2):
                backward_block(i, 2 * p + u)
        each(t % 2 * (n_pairs // 4), (t % 2 + 1) * (n_pairs // 4), one)

        @pl.when(t % 2 == 1)
        def _():
            for h in range(2):
                group_sums(h, chunk, 2 * two + h)
        for step in sorted(after):
            @pl.when(t == step)
            def _(step=step):
                run(in_order(after[step]))

    each(0, n_slots, slot)
    run(in_order(late))
    sm_ref[...] = fin[...]

    w_own().wait_send()
    for k in range(1, pairs):
        for h in range(2):
            w_x(k, h).wait_send()
            for o in range(n_y):
                w_z(k, h, o).wait_send()
            for o in range(1, n_y):
                w_y(k, h, o).wait_send()
        for h in range(2):
            for zz in range(2):
                each(0, n_y, lambda a: w_fw(k, a, zz, h).wait_send())
        for n in range(len(units)):
            each(0, n_y, lambda a: t_x(k, n, a).wait_send())
    for k in range(pairs):
        each(0, gpc, lambda q: t_core(k, q).wait_send())

    for n in range(len(units)):
        for o in range(1, n_y):
            all_yr(n, o).wait_send()
            all_ya(n, o).wait_send()
        if len(T_UNIT[n + 5 - len(units)]) == 5:
            for o in range(1, n_z):
                t_zr(n, o).wait_send()
                t_za(n, o).wait_send()
        else:
            for m in range(half_z):
                t_zp(n, m).wait_send()
                t_ap(n, m).wait_send()
            for m in range(1, half_z):
                t_zc(n, m).wait_send()
                t_za(n, 2 * m).wait_send()
    for k in range(pairs):
        for j in range(2):
            t_sa(k, j).wait_send()
    if n_own == n_chips:
        each(0, n_dp, lambda chunk: all_sb(chunk).wait_send())
    else:
        each(0, n_dp, lambda chunk: each(1, n_chips, lambda o: owner((chip + o) % n_chips, lambda: t_sb(chunk, o).wait_send())))
    for j in range(2):
        if n_own == n_chips:
            all_sc(j).wait_send()
        else:
            owner(chip, lambda: each(1, n_chips, lambda o: t_sc(j, o).wait_send()))
        t_sd(j).wait_send()


def finish(dims, gu_ref, gv_ref, dw_ref, sm_ref, gu_hbm, gv_hbm, dw_hbm, gw_hbm, bias_ref, gain_ref, shift_ref, dw_f, gw_f, sem, dw_sem):
    gpc, span, chans, width, n_sp, groups, prow = dims
    copies = [
        pltpu.make_async_copy(gu_ref, gu_hbm.at[0], sem.at[0]),
        pltpu.make_async_copy(gv_ref, gv_hbm.at[0], sem.at[1]),
    ]
    for copy in copies:
        copy.start()
    for q in range(gpc):
        for j in range(n_sp):
            dw_f[q * span : (q + 1) * span, j * width : (j + 1) * width] = dw_ref[q, j].astype(F32)
        at = pl.ds(q * span, span)
        copy = pltpu.make_async_copy(dw_f.at[at], dw_hbm.at[at], dw_sem.at[q])
        copy.start()
        copies.append(copy)
    r = lax.broadcasted_iota(jnp.int32, (prow, chans), 0)
    l = lax.broadcasted_iota(jnp.int32, (prow, chans), 1)
    per = span // prow
    hq = gpc // 2
    for g in range(groups):
        chunk, q = divmod(g, gpc)
        xx, j = divmod(chunk, 2)
        for p in range(per):
            block = sm_ref[j, q // hq, q % hq * per + p, xx].astype(F32)
            gw_f[g, p * prow : (p + 1) * prow, :] = jnp.where(r + p * prow >= l, block, 0.0)
            if p == 0:
                turned = pltpu.roll(block[:8], chans // 2, 1)
                for n, ref in enumerate((bias_ref, gain_ref, shift_ref)):
                    ref[g : g + 1, :] = jnp.where(l[:1] < chans // 2, turned[n : n + 1], block[n + 3 : n + 4])
    copy = pltpu.make_async_copy(gw_f, gw_hbm, sem.at[2])
    copy.start()
    copies.append(copy)
    for copy in copies:
        copy.wait()


def on_device(n_sp, n_dp, u_pre, v_pre, d_out, w_mix, mix_bias, norm_gain, norm_shift, w_out):
    _, rows, wide = u_pre.shape
    depth = d_out.shape[2]
    groups, span = w_mix.shape[:2]
    chans = wide // groups
    gpc = groups // n_dp
    width = depth // n_sp
    shard = w_out.shape[0]
    pairs = n_dp // 2
    n_chips = n_sp * pairs
    half_rows = gpc // 2 * span
    prow = max(16, half_rows // n_chips)
    n_own = half_rows // prow
    n_y = 1
    while 4 * n_y * n_y <= n_sp:
        n_y *= 2
    n_z = n_sp // n_y
    dims = (n_y, n_z, n_dp, gpc, span, chans, width, rows, prow, n_own)
    dma = pltpu.SemaphoreType.DMA
    vm = pltpu.VMEM
    piece = (n_y, n_z, span, width)
    w_piece = (n_y, 2, 2, shard // (4 * n_y), depth)
    scratch = [
        vm((rows, wide), BF16), vm((rows, wide), BF16), vm((rows, depth), BF16),
        vm((groups, span, span), BF16),
        vm((groups, 1, span), F32), vm((groups, 1, chans), F32), vm((groups, 1, chans), F32),
        vm((groups, span, chans), F32),
        dma((pairs,)), dma((pairs,)), dma((6,)),
        vm((n_dp,) + w_piece, BF16),
        vm((groups,) + piece, BF16),
        vm((pairs, gpc) + piece, BF16),
        vm((pairs - 1, gpc) + piece, BF16),
        vm((gpc, n_y - 1) + piece[1:], BF16),
        vm((gpc, n_z - 1) + piece[2:], BF16),
        vm((gpc,) + piece, BF16),
        vm((2, rows, 2 * chans), BF16),
        vm((2, 2 * chans, rows), BF16),
        vm((2, span, span), BF16),
        vm((2, span, span), BF16),
        vm((2, 4, span, chans), F32),
        vm((n_dp, 2, n_own, prow, chans), BF16),
        vm((n_dp, n_own, prow, chans), BF16),
        vm((n_dp, n_chips - 1, prow, chans), BF16),
        vm((2, 2, n_own, pairs, prow, chans), BF16),
        dma, dma,
        dma((pairs, 2)), dma((pairs, 2)),
        dma((pairs, 2, n_y)), dma((pairs, 2, n_y)),
        dma((pairs, 2, n_y)), dma((pairs, 2, n_y)),
        dma((pairs, n_y, 2, 2)), dma((pairs, n_y, 2, 2)),
        dma((pairs, gpc)), dma((pairs, gpc)),
        dma((pairs, gpc + 1, n_y)), dma((pairs, gpc + 1, n_y)),
        dma((gpc + 1, n_y)), dma((gpc + 1, n_y, n_z)),
        dma((gpc + 1, n_z)), dma((gpc + 1, n_z)),
        dma((gpc + 1, n_z)), dma((gpc + 1, n_z)),
        dma((gpc + 1, n_y)), dma((gpc + 1, n_y)),
        dma((n_dp,)), dma((n_dp,)),
        dma((n_dp,)), dma((n_dp,)),
        dma((2,)), dma((2,)),
        dma((2,)), dma((2,)),
    ]
    spec = pl.BlockSpec(memory_space=pltpu.VMEM)
    hbm = pl.BlockSpec(memory_space=pl.ANY)
    results = pl.pallas_call(
        functools.partial(kernel, dims),
        out_shape=(
            vm((rows, wide), BF16),
            vm((rows, wide), BF16),
            vm((gpc, n_sp, span, width), BF16),
            vm((2, 2, n_own, pairs, prow, chans), BF16),
        ),
        in_specs=[hbm] * 8,
        out_specs=(spec,) * 4,
        scratch_shapes=scratch,
        compiler_params=pltpu.CompilerParams(
            collective_id=0, has_side_effects=True, vmem_limit_bytes=48 * 1024 * 1024,
        ),
    )(
        u_pre[0], v_pre[0], d_out[0], w_mix,
        mix_bias[:, None, :], norm_gain[:, None, :], norm_shift[:, None, :],
        w_out.reshape(w_piece),
    )
    return pl.pallas_call(
        functools.partial(finish, (gpc, span, chans, width, n_sp, groups, prow)),
        out_shape=(
            jax.ShapeDtypeStruct((1, rows, wide), BF16),
            jax.ShapeDtypeStruct((1, rows, wide), BF16),
            jax.ShapeDtypeStruct((shard, depth), F32),
            jax.ShapeDtypeStruct((groups, span, span), F32),
            jax.ShapeDtypeStruct((groups, span), F32),
            jax.ShapeDtypeStruct((groups, chans), F32),
            jax.ShapeDtypeStruct((groups, chans), F32),
        ),
        in_specs=[spec] * 4,
        out_specs=(hbm,) * 4 + (spec,) * 3,
        scratch_shapes=[
            vm((shard, depth), F32), vm((groups, span, span), F32), dma((3,)), dma((gpc,)),
        ],
        compiler_params=pltpu.CompilerParams(vmem_limit_bytes=32 * 1024 * 1024),
    )(*[pltpu.with_memory_space_constraint(r, pltpu.VMEM) for r in results])


def solution(mesh):
    body = functools.partial(on_device, mesh.shape["sp"], mesh.shape["dp"])
    return jax.shard_map(
        body,
        mesh=mesh,
        in_specs=(
            P("dp", "sp", None),
            P("dp", "sp", None),
            P("dp", "sp", None),
            P(),
            P(),
            P(),
            P(),
            P("dp", None),
        ),
        out_specs=(P("dp", "sp", None), P("dp", "sp", None), P("dp", None), P(), P(), P(), P()),
        check_vma=False,
    )
```

```python
import functools

import jax
import jax.numpy as jnp
from jax import lax
from jax.experimental import pallas as pl
from jax.experimental.pallas import tpu as pltpu
from jax.sharding import PartitionSpec as P

EPS = 1e-05
K0 = 0.7978845608028654
K1 = 0.044715
F32 = jnp.float32
BF16 = jnp.bfloat16


TIMES = (6.0, 2.4, 27.7, 2.05, 6, 2.5)
T_W = (13.5, 19.5, 21.6, 27.0)
T_WZ = ((0, 2), (3, 5))
T_UNIT = (
    (25.0, 33.5, 43.0, 50.5, 56.8, 64.9, 80.7),
    (37.0, 46.2, 52.0, 58.2, 64.85, 69.5, 80.8),
    (48.0, 56.6, 64.4, 72.0, 84.0),
    (56.5, 62.8, 69.0, 75.0, 83.0),
    (64.0, 69.3, 75.2, 80.4, 86.0),
)
T_END = (64.6, 64.8, 70.0, 76.0, 81.0, 69.7, 75.5, 80.5, 85.5)


def gelu_parts(a):
    sq = a * a
    t = jnp.tanh(a * (K0 + (K0 * K1) * sq))
    half = 0.5 * (1.0 + t)
    return sq, t, half


def gelu(a):
    _, _, half = gelu_parts(a)
    return a * half


def gelu_both(a):
    sq, t, half = gelu_parts(a)
    slope = half + (0.5 * a) * (1.0 - t * t) * (K0 + (3.0 * K0 * K1) * sq)
    return a * half, slope


def norm_parts(gated):
    centre = gated - jnp.mean(gated, axis=-1, keepdims=True)
    inverse = lax.rsqrt(jnp.mean(centre * centre, axis=-1, keepdims=True) + EPS)
    return centre * inverse, inverse


def mm(a, b, ca, cb):
    return lax.dot_general(a, b, (((ca,), (cb,)), ((), ())), preferred_element_type=F32)


def each(lo, hi, fn):
    def body(i, carry):
        fn(i)
        return carry
    lax.fori_loop(lo, hi, body, 0)


def kernel(
    dims,
    u_hbm, v_hbm, d_hbm, wmix_hbm, bias_hbm, gain_hbm, shift_hbm, w_hbm,
    gu_ref, gv_ref, dw_ref, sm_ref,
    u_ref, v_ref, d_ref, wmix_ref, bias_row, gain_ref, shift_ref, bias_ref, u_s, v_s, in_s,
    wfull, part, rcore, rx, ry, rz, ag, gs, got, wl_ref, wlt_ref, acc,
    sbuf, acore, s1r, s2r, fin,
    wown_s, wown_r, wx_s, wx_r, wy_s, wy_r, wz_s, wz_r, wfw_s, wfw_r,
    core_s, core_r, xs_s, xs_r, yr_s, yr_r, zr_s, zr_r, za_s, za_r, ya_s, ya_r,
    sa_s, sa_r, s1_s, s1_r, s2_s, s2_r, s3_s, s3_r, s4_s, s4_r, sd_s, sd_r,
):
    n_y, n_z, n_dp, gpc, span, chans, width, rows, prow, n_own = dims
    n_sp = n_y * n_z
    pairs = n_dp // 2
    n_chips = n_sp * pairs
    nb = rows // span
    s = lax.axis_index("sp")
    dpi = lax.axis_index("dp")
    x = dpi // 2
    c = dpi % 2
    y = s % n_y
    z = s // n_y
    zp = z % 2
    other = 1 - c
    mate = {"sp": s, "dp": 2 * x + other}
    n_pl = n_y * pairs
    plane = y * pairs + x
    chip = plane * n_z + z
    own_pl = max(1, n_own // n_z)
    full = own_pl == n_pl

    def rc(src, dst, ssem, rsem, dev):
        return pltpu.make_async_remote_copy(
            src_ref=src, dst_ref=dst, send_sem=ssem, recv_sem=rsem,
            device_id=dev, device_id_type=pl.DeviceIdType.MESH,
        )

    def up(k):
        return (x + k) % pairs

    def down(k):
        return (x + pairs - k) % pairs

    def at_x(k):
        return {"sp": s, "dp": 2 * up(k) + c}

    def at_y(o):
        return {"sp": z * n_y + (y + o) % n_y, "dp": dpi}

    def at_z(o):
        return {"sp": (z + o) % n_z * n_y + y, "dp": dpi}

    def at_plane(o):
        to = (plane + o) % n_pl
        return {"sp": z * n_y + to // pairs, "dp": 2 * (to % pairs) + c}

    def w_own():
        return rc(wfull.at[dpi], wfull.at[dpi], wown_s, wown_r, mate)

    def w_x(k, h):
        block = wfull.at[dpi, y, zp, h]
        return rc(block, block, wx_s.at[k - 1], wx_r.at[k - 1, h], at_x(k))

    def w_y(k, h, o):
        block = wfull.at[2 * down(k) + c, y, zp, h]
        return rc(block, block, wy_s.at[k - 1, o - 1], wy_r.at[k - 1, h, o - 1], at_y(o))

    def w_z(k, h, o):
        a = (y + o) % n_y
        block = wfull.at[2 * down(k) + c, a, zp, h]
        to = {"sp": (z + 1 - 2 * zp) * n_y + y, "dp": dpi}
        return rc(block, block, wz_s.at[k - 1], wz_r.at[k - 1, h, o], to)

    def w_fw(k, a, zz, h):
        block = wfull.at[2 * down(k) + c, a, zz, h]
        return rc(block, block, wfw_s.at[k - 1], wfw_r.at[k - 1], mate)

    def sized(ref, ssem, rsem):
        return rc(ref, ref, ssem, rsem, mate)

    units = [(q, 0, span) for q in range(gpc - 1)]
    units += [(gpc - 1, 0, span // 2), (gpc - 1, span // 2, span // 2)]
    half_z = n_z // 2

    def gid(xx, cc, q):
        return (2 * xx + cc) * gpc + q

    def t_core(k, q):
        return rc(part.at[gid(up(k), other, q)], rcore.at[k, q], core_s.at[k], core_r.at[k, q], mate)

    def t_x(k, n, a):
        q, lo, size = units[n]
        at = pl.ds(lo, size)
        return rc(
            part.at[gid(up(k), c, q), a, :, at], rx.at[k - 1, q, a, :, at],
            xs_s.at[k - 1], xs_r.at[k - 1, n, a], at_x(k),
        )

    def t_yr(n, o, b):
        q, lo, size = units[n]
        at = pl.ds(lo, size)
        return rc(
            part.at[gid(x, c, q), (y + o) % n_y, b, at], ry.at[q, o - 1, b, at],
            yr_s.at[o - 1], yr_r.at[n, o - 1, b], at_y(o),
        )

    def z_send(n, b, slot, dst_slot, to):
        q, lo, size = units[n]
        at = pl.ds(lo, size)
        return rc(
            part.at[gid(x, c, q), y, b, at], rz.at[q, dst_slot, at],
            zr_s, zr_r.at[n, slot - 1], to,
        )

    to_pair = {"sp": (z + 1 - 2 * zp) * n_y + y, "dp": dpi}
    pair_z = z + 1 - 2 * zp

    def t_zr(n, o):
        return z_send(n, (z + o) % n_z, o, o - 1, at_z(o))

    def t_zp(n, m):
        return z_send(n, (pair_z + 2 * m) % n_z, 2 * m + 1, m, to_pair)

    def t_zc(n, m):
        return z_send(n, (z + 2 * m) % n_z, 2 * m, half_z + m - 1, at_z(2 * m))

    def gathered(n, b, ssem, rsem, to):
        q, lo, size = units[n]
        block = ag.at[q, y, b, pl.ds(lo, size)]
        return rc(block, block, ssem, rsem, to)

    def t_za(n, o):
        return gathered(n, z, za_s, za_r.at[n, o - 1], at_z(o))

    def t_ap(n, m):
        return gathered(n, (z + 2 * m) % n_z, za_s, za_r.at[n, 2 * m], to_pair)

    def t_ya(n, o, b):
        return gathered(n, b, ya_s.at[o - 1], ya_r.at[n, o - 1], at_y(o))

    def all_ya(n, o):
        q, lo, size = units[n]
        block = ag.at[q, y, :, pl.ds(lo, size)]
        return sized(block, ya_s.at[o - 1], ya_r.at[n, o - 1])

    def t_sa(k, j):
        chunk = 2 * down(k) + j
        return rc(sbuf.at[chunk, other], acore.at[chunk], sa_s, sa_r.at[chunk], mate)

    def pieces(to):
        return pl.ds(to % own_pl * n_z, n_z)

    def t_s1(chunk, o):
        to = (plane + o) % n_pl
        return rc(sbuf.at[chunk, c, pieces(to)], s1r.at[chunk, o - 1], s1_s.at[chunk], s1_r.at[chunk], at_plane(o))

    def t_s2(chunk, o):
        to = plane % own_pl * n_z + (z + o) % n_z
        return rc(sbuf.at[chunk, c, to], s2r.at[chunk, o - 1], s2_s.at[chunk], s2_r.at[chunk], at_z(o))

    def t_s3(j, o):
        block = fin.at[j, c, plane % own_pl * n_z + z]
        return rc(block, block, s3_s.at[j], s3_r.at[j], at_z(o))

    def t_s4(j, o):
        block = fin.at[j, c, pieces(plane)]
        return rc(block, block, s4_s.at[j], s4_r.at[j], at_plane(o))

    def t_sd(j):
        return rc(fin.at[j, c], fin.at[j, c], sd_s.at[j], sd_r.at[j], mate)

    def all_s1(chunk):
        return sized(s1r.at[chunk], s1_s.at[chunk], s1_r.at[chunk])

    def all_s2(chunk):
        return sized(s2r.at[chunk], s2_s.at[chunk], s2_r.at[chunk])

    def all_s3(j):
        return sized(fin.at[j, c, pl.ds(0, n_z - 1)], s3_s.at[j], s3_r.at[j])

    def all_s4(j):
        return sized(fin.at[j, c, pl.ds(0, (n_pl - 1) * n_z)], s4_s.at[j], s4_r.at[j])

    def owner(t, fn):
        if full:
            fn()
        else:
            pl.when(t < own_pl)(fn)

    row = lax.broadcasted_iota(jnp.int32, (span, span), 0)
    col = lax.broadcasted_iota(jnp.int32, (span, span), 1)
    lower = row >= col
    share = 2 * gpc * chans

    def cols(k):
        return pl.ds(pl.multiple_of(up(k) * share, share), share)

    small = [
        pltpu.make_async_copy(src, dst, in_s.at[n])
        for n, (src, dst) in enumerate((
            (bias_hbm, bias_row), (gain_hbm, gain_ref), (shift_hbm, shift_ref), (wmix_hbm, wmix_ref),
        ))
    ]
    near = {k: (
        pltpu.make_async_copy(v_hbm.at[:, cols(k)], v_ref.at[:, cols(k)], v_s.at[k]),
        pltpu.make_async_copy(u_hbm.at[:, cols(k)], u_ref.at[:, cols(k)], u_s.at[k]),
    ) for k in range(pairs)}
    first_k = 1 % pairs
    load_w = pltpu.make_async_copy(w_hbm, wfull.at[dpi], in_s.at[4])
    load_d = pltpu.make_async_copy(d_hbm, d_ref, in_s.at[5])
    for load in small:
        load.start()
    for load in near[first_k]:
        load.start()
    load_w.start()
    load_d.start()
    for k in range(pairs):
        if k != first_k:
            for load in near[k]:
                load.start()
    barrier = pltpu.get_barrier_semaphore()
    pl.semaphore_signal(barrier, inc=1, device_id=mate, device_id_type=pl.DeviceIdType.MESH)
    for o in range(1, n_pl):
        pl.semaphore_signal(barrier, inc=1, device_id=at_plane(o), device_id_type=pl.DeviceIdType.MESH)
    for o in range(1, n_z):
        pl.semaphore_signal(barrier, inc=1, device_id=at_z(o), device_id_type=pl.DeviceIdType.MESH)

    def lanes(g):
        return pl.ds(pl.multiple_of(g * chans, chans), chans)

    def far_group(i, h):
        return gid(up((i // gpc + 1) % pairs), (c + h) % 2, i % gpc)

    def low_weights(g, h):
        wl_ref[h] = jnp.where(lower, wmix_ref[g], jnp.zeros((), BF16))

    def forward_block(i, b):
        at = pl.ds(pl.multiple_of(b * span, span), span)
        for h in range(2):
            g = far_group(i, h)
            scaled, _ = norm_parts(gelu(v_ref[at, lanes(g)].astype(F32)))
            normed = (scaled * gain_ref[g] + shift_ref[g]).astype(BF16)
            mixed = mm(wl_ref[h], normed, 1, 0) + bias_ref[g]
            out = (gelu(u_ref[at, lanes(g)].astype(F32)) * mixed).astype(BF16)
            got[i % 2, h * span : (h + 1) * span, at] = out.T

    def core_sum(k, q):
        t_core(k, q).wait_recv()
        g = gid(up(k), c, q)

        def one(j):
            a, b = j // n_z, j % n_z
            part[g, a, b] = (part[g, a, b].astype(F32) + rcore[k, q, a, b].astype(F32)).astype(BF16)
        each(0, n_sp, one)

    def x_start(k, n):
        for o in range(n_y):
            t_x(k, n, (y + 1 + o) % n_y).start()

    per_block = n_sp // nb

    def product_block(i, b):
        keep = far_group(i, 0)
        give = far_group(i, 1)
        wide = per_block * width
        r = mm(got[i % 2], d_ref[:, pl.ds(pl.multiple_of(b * wide, wide), wide)], 1, 0)
        for e in range(per_block):
            j = b * per_block + e
            at = slice(e * width, (e + 1) * width)
            part[keep, j // n_z, j % n_z] = r[:span, at].astype(BF16)
            part[give, j // n_z, j % n_z] = r[span:, at].astype(BF16)

    def give_core(i):
        t_core((i // gpc + 1) % pairs, i % gpc).start()

    def w_from_x(h):
        for k in range(1, pairs):
            w_x(k, h).wait_recv()
            for o in range(1, n_y):
                w_y(k, h, o).start()
            w_z(k, h, 0).start()
            w_fw(k, y, zp, h).start()

    def w_from_y(h):
        for k in range(1, pairs):
            for o in range(1, n_y):
                w_y(k, h, o).wait_recv()
            for o in range(1, n_y):
                w_z(k, h, o).start()
                w_fw(k, (y + o) % n_y, zp, h).start()

    def w_from_z(h, o):
        for k in range(1, pairs):
            w_z(k, h, o).wait_recv()
            w_fw(k, (y + o) % n_y, 1 - zp, h).start()

    def w_ready(k):
        sized(wfull.at[2 * down(k) + other], wfw_s.at[k - 1], wfw_r.at[k - 1]).wait_recv()

    def yr_start(n):
        q, lo, size = units[n]
        if lo == 0:
            t_core(0, q).wait_recv()
        at = pl.ds(lo, size)
        g = gid(x, c, q)
        for o in range(1, n_y):
            a = (y + o) % n_y
            for k in range(1, pairs):
                t_x(k, n, a).wait_recv()

            def one(b):
                total = part[g, a, b, at].astype(F32) + rcore[0, q, a, b, at].astype(F32)
                for k in range(1, pairs):
                    total = total + rx[k - 1, q, a, b, at].astype(F32)
                part[g, a, b, at] = total.astype(BF16)
                t_yr(n, o, b).start()
            each(1, n_z + 1, lambda j: one((z + j) % n_z))

    def own_total(n, b):
        q, lo, size = units[n]
        at = pl.ds(lo, size)
        total = part[gid(x, c, q), y, b, at].astype(F32) + rcore[0, q, y, b, at].astype(F32)
        for k in range(1, pairs):
            total = total + rx[k - 1, q, y, b, at].astype(F32)
        for o in range(1, n_y):
            total = total + ry[q, o - 1, b, at].astype(F32)
        return total

    def own_ready(n):
        for k in range(1, pairs):
            t_x(k, n, y).wait_recv()

    def y_ready(n, b):
        for o in range(1, n_y):
            t_yr(n, o, b).wait_recv()

    def keep_sum(n, b, total):
        q, lo, size = units[n]
        part[gid(x, c, q), y, b, pl.ds(lo, size)] = total.astype(BF16)

    def from_z(n, slot):
        q, lo, size = units[n]
        return rz[q, slot, pl.ds(lo, size)].astype(F32)

    def whole(n, total):
        q, lo, size = units[n]
        ag[q, y, z, pl.ds(lo, size)] = total.astype(BF16)
        for o in range(1, n_y):
            t_ya(n, o, z).start()

    def zr_start(n):
        own_ready(n)
        for j in range(1, n_z):
            b = (z + j) % n_z
            y_ready(n, b)
            keep_sum(n, b, own_total(n, b))
            t_zr(n, j).start()

    def za_start(n):
        y_ready(n, z)
        total = own_total(n, z)
        for o in range(1, n_z):
            t_zr(n, o).wait_recv()
            total = total + from_z(n, o - 1)
        whole(n, total)
        for o in range(1, n_z):
            t_za(n, o).start()

    def ya_start(n):
        for o in range(1, n_z):
            t_za(n, o).wait_recv()
            for a in range(1, n_y):
                t_ya(n, a, (z + n_z - o) % n_z).start()

    def zp_start(n):
        own_ready(n)
        for j in range(half_z):
            m = half_z - 1 - j
            b = (pair_z + 2 * m) % n_z
            y_ready(n, b)
            keep_sum(n, b, own_total(n, b))
            t_zp(n, m).start()

    def zc_start(n):
        for m in range(1, half_z):
            b = (z + 2 * m) % n_z
            y_ready(n, b)
            t_zp(n, m).wait_recv()
            keep_sum(n, b, own_total(n, b) + from_z(n, m))
            t_zc(n, m).start()

    def ac_start(n):
        y_ready(n, z)
        t_zp(n, 0).wait_recv()
        total = own_total(n, z) + from_z(n, 0)
        for m in range(1, half_z):
            t_zc(n, m).wait_recv()
            total = total + from_z(n, half_z + m - 1)
        whole(n, total)
        for m in range(1, half_z):
            t_za(n, 2 * m).start()
        t_ap(n, 0).start()

    def ap_start(n):
        for m in range(1, half_z):
            t_za(n, 2 * m).wait_recv()
            t_ap(n, half_z - m).start()
            for a in range(1, n_y):
                t_ya(n, a, (z + n_z - 2 * m) % n_z).start()

    def yb_start(n):
        for m in range(half_z):
            t_ap(n, m).wait_recv()
            for a in range(1, n_y):
                t_ya(n, a, (pair_z + 2 * m) % n_z).start()

    def dw_done(n):
        q, lo, size = units[n]
        for o in range(1, n_y):
            all_ya(n, o).wait_recv()

        def one(j):
            dw_ref[q, j, pl.ds(lo, size)] = ag[q, j // n_z, j % n_z, pl.ds(lo, size)]
        each(0, n_sp, one)

    def bias_column(g):
        bias_ref[g] = jnp.broadcast_to(bias_row[g], (span, span)).T

    for load in small:
        load.wait()
    each(0, n_dp * gpc, lambda g: bias_column(g))
    for load in near[first_k]:
        load.wait()
    for h in range(2):
        low_weights(far_group(0, h), h)

    def first_blocks(b):
        for n in range(4):
            forward_block(0, 4 * b + n)
    each(0, nb // 4, first_blocks)
    load_w.wait()
    pl.semaphore_wait(barrier, n_pl + n_z - 1)
    for h in range(2):
        for k in range(1, pairs):
            w_x(k, h).start()
    w_own().start()
    load_d.wait()
    for k in range(pairs):
        if k != first_k:
            for load in near[k]:
                load.wait()

    n_far = (pairs - 1) * gpc
    n_fwd = pairs * gpc
    per_chunk = gpc // 2
    n_steps = n_dp * per_chunk
    n_slots = 2 * n_steps
    before = {}
    after = {}
    late = []

    def run(todo):
        for fn, args in todo:
            fn(*args)

    def sa_start(k, j):
        t_sa(k, j).start()

    def s1_start(k, j):
        t_sa(k, j).wait_recv()
        chunk = 2 * down(k) + j

        def one(p):
            sbuf[chunk, c, p] = (sbuf[chunk, c, p].astype(F32) + acore[chunk, p].astype(F32)).astype(BF16)
        each(0, n_own, one)
        for o in range(1, n_pl):
            owner((plane + o) % n_pl, lambda o=o: t_s1(chunk, o).start())

    def s2_start(j):
        def mine():
            for xx in range(pairs):
                chunk = 2 * xx + j
                all_s1(chunk).wait_recv()

                def one(n, chunk=chunk):
                    p = plane % own_pl * n_z + n
                    total = sbuf[chunk, c, p].astype(F32)
                    for o in range(1, n_pl):
                        total = total + s1r[chunk, o - 1, n].astype(F32)
                    sbuf[chunk, c, p] = total.astype(BF16)
                each(0, n_z, one)
                for o in range(1, n_z):
                    t_s2(chunk, o).start()
        owner(plane, mine)

    def s3_start(j):
        def mine():
            p = plane % own_pl * n_z + z
            for xx in range(pairs):
                chunk = 2 * xx + j
                all_s2(chunk).wait_recv()
                total = sbuf[chunk, c, p].astype(F32)
                for o in range(1, n_z):
                    total = total + s2r[chunk, o - 1].astype(F32)
                fin[j, c, p, xx] = total.astype(BF16)
            for o in range(1, n_z):
                t_s3(j, o).start()
        owner(plane, mine)

    def s4_start(j):
        def mine():
            all_s3(j).wait_recv()
            for o in range(1, n_pl):
                t_s4(j, o).start()
        owner(plane, mine)

    def sd_start(j):
        if full:
            all_s4(j).wait_recv()
        else:
            for o in range(1, n_pl):
                owner((plane + n_pl - o) % n_pl, lambda o=o: t_s4(j, o).wait_recv())
        t_sd(j).start()

    fwd_0, fwd_us, bwd_0, bwd_us, pause_at, pause_us = TIMES

    def put(time, fn, *args):
        step = 0
        while step <= n_fwd and fwd_0 + fwd_us * step < time:
            step += 1
        at_slot = 0
        while at_slot < n_slots and bwd_0 + bwd_us * (at_slot + 1) + pause_us * (at_slot >= pause_at) < time:
            at_slot += 1
        if step <= n_fwd:
            before.setdefault(max(step, 1), []).append((time, fn, args))
        elif at_slot < n_slots:
            after.setdefault(at_slot, []).append((time, fn, args))
        else:
            late.append((time, fn, args))

    def put_slot(at_slot, time, fn, *args):
        if at_slot < n_slots:
            after.setdefault(at_slot, []).append((time, fn, args))
        else:
            late.append((time, fn, args))

    def in_order(todo):
        return [(fn, args) for _, fn, args in sorted(todo, key=lambda item: item[0])]

    put(T_W[0], w_from_x, 0)
    put(T_W[1], w_from_x, 1)
    put(T_W[2], w_from_y, 0)
    put(T_W[3], w_from_y, 1)
    need = 4 * per_chunk - 3
    for h in range(2):
        for o in range(n_y):
            put_slot(min(need, T_WZ[min(o, 1)][h]), 0.0 + o + h / 2, w_from_z, h, o)
    pair_stages = (yr_start, zp_start, zc_start, ac_start, ap_start, yb_start, dw_done)
    line_stages = (yr_start, zr_start, za_start, ya_start, dw_done)
    for n in range(len(units)):
        when = T_UNIT[n + 5 - len(units)]
        stages = line_stages if len(when) == 5 else pair_stages
        for fn, time in zip(stages, when):
            put(time, fn, n)
    for turn in range(n_dp):
        end = 2 * (turn + 1) * per_chunk
        put_slot(end - 1, 0.0, sa_start, turn // 2, turn % 2)
        put_slot(end, 0.5 if end < n_slots else T_END[0], s1_start, turn // 2, turn % 2)
    for j in range(2):
        for fn, time in zip((s2_start, s3_start, s4_start, sd_start), T_END[1 + 4 * j : 5 + 4 * j]):
            put(time, fn, j)

    def sd_done():
        for j in range(2):
            t_sd(j).wait_recv()
    put(1000.0, sd_done)

    def core_sums(last):
        @pl.when((last >= 0) & (last < n_far))
        def _():
            k = (last // gpc + 1) % pairs
            core_sum(k, last % gpc)
            for kk in range(1, pairs):
                for n, unit in enumerate(units):
                    @pl.when(last == (kk - 1) * gpc + unit[0])
                    def _(kk=kk, n=n):
                        x_start(kk, n)

    def forward_step(i):
        for h in range(2):
            low_weights(far_group(i, h), h)

        def one(b):
            for n in range(4):
                product_block(i - 1, 4 * b + n)
            for n in range(4):
                forward_block(i, 4 * b + n)
        each(0, nb // 4, one)
        give_core(i - 1)
        core_sums(i - 2)
        for step in sorted(before):
            @pl.when(i == step)
            def _(step=step):
                run(in_order(before[step]))

    each(1, n_fwd, forward_step)
    each(0, nb, lambda b: product_block(n_fwd - 1, b))
    give_core(n_fwd - 1)
    core_sums(n_fwd - 2)
    core_sums(n_fwd - 1)
    w_own().wait_recv()
    run(in_order(before.get(n_fwd, [])))

    def backward_block(i, p):
        chunk, two = place(i)
        first = chunk * gpc + 2 * two
        for h in range(2):
            g = first + h
            gain = gain_ref[g]
            for e in range(2):
                at = pl.ds(pl.multiple_of((2 * p + e) * span, span), span)
                gated, v_slope = gelu_both(v_ref[at, lanes(g)].astype(F32))
                scaled, inverse = norm_parts(gated)
                normed = (scaled * gain + shift_ref[g]).astype(BF16)
                mixed = mm(wl_ref[h], normed, 1, 0) + bias_ref[g]
                upper, u_slope = gelu_both(u_ref[at, lanes(g)].astype(F32))
                cot = gs[i % 2, at, h * chans : (h + 1) * chans].astype(F32)
                dm = cot * upper
                dmb = dm.astype(BF16)
                gu_ref[at, lanes(g)] = (cot * mixed * u_slope).astype(BF16)
                acc[h, 0] += dm
                acc[h, 1] += mm(dmb, normed, 1, 1)
                dn = mm(wlt_ref[h], dmb, 1, 0)
                acc[h, 2] += dn * scaled
                acc[h, 3] += dn
                e_ = dn * gain
                m1 = jnp.mean(e_, axis=-1, keepdims=True)
                m2 = jnp.mean(e_ * scaled, axis=-1, keepdims=True)
                gv_ref[at, lanes(g)] = (v_slope * (inverse * (e_ - m1 - scaled * m2))).astype(BF16)

    def group_sums(h, chunk, q):
        grad_w = jnp.where(lower, acc[h, 1], 0.0)
        g_bias = jnp.sum(acc[h, 0].T, axis=0, keepdims=True)
        g_gain = jnp.sum(acc[h, 2], axis=0, keepdims=True)
        g_shift = jnp.sum(acc[h, 3], axis=0, keepdims=True)
        r16 = lax.broadcasted_iota(jnp.int32, (16, chans), 0)
        c16 = lax.broadcasted_iota(jnp.int32, (16, chans), 1)
        extra = jnp.where(r16 % 3 == 0, g_bias, jnp.where(r16 % 3 == 1, g_gain, g_shift))
        turned = pltpu.roll(extra, chans // 2, 1)
        top = jnp.where(c16 < chans // 2, grad_w[:16], jnp.where(r16 < 3, turned, jnp.where(r16 < 6, extra, 0.0)))
        per = span // prow
        hq = gpc // 2
        first = q % hq * per
        for p in range(per):
            block = grad_w[p * prow : (p + 1) * prow]
            if p == 0:
                block = jnp.concatenate([top, block[16:]], axis=0) if prow > 16 else top
            sbuf[chunk, q // hq, first + p] = block.astype(BF16)

    flat = wfull.reshape(n_dp, wfull.shape[1] * wfull.shape[2] * wfull.shape[3] * wfull.shape[4], wfull.shape[5])

    def place(i):
        turn = i // per_chunk
        return 2 * down(turn // 2) + turn % 2, i % per_chunk

    def cotangent_block(i, p):
        chunk, two = place(i)
        at = pl.ds(pl.multiple_of(p * 2 * span, 2 * span), 2 * span)
        these = pl.ds(pl.multiple_of(two * 2 * span, 2 * span), 2 * span)
        gs[i % 2, at, :] = mm(d_ref[at, :], flat[chunk, these, :], 1, 1).astype(BF16)

    n_pairs = nb // 2
    each(0, n_pairs, lambda p: cotangent_block(0, p))

    def slot(t):
        i = t // 2
        chunk, two = place(i)

        @pl.when(t % 2 == 0)
        def _():
            for k in range(1, pairs):
                @pl.when(i + 1 == 2 * k * per_chunk)
                def _(k=k):
                    w_ready(k)
            acc[...] = jnp.zeros_like(acc)
            for h in range(2):
                low_weights(chunk * gpc + 2 * two + h, h)
                wlt_ref[h] = wl_ref[h].T

        def one(p):
            for u in range(2):
                cotangent_block((i + 1) % n_steps, 2 * p + u)
            for u in range(2):
                backward_block(i, 2 * p + u)
        each(t % 2 * (n_pairs // 4), (t % 2 + 1) * (n_pairs // 4), one)

        @pl.when(t % 2 == 1)
        def _():
            for h in range(2):
                group_sums(h, chunk, 2 * two + h)
        for step in sorted(after):
            @pl.when(t == step)
            def _(step=step):
                run(in_order(after[step]))

    each(0, n_slots, slot)
    run(in_order(late))
    sm_ref[...] = fin[...]

    w_own().wait_send()
    for k in range(1, pairs):
        mine = wfull.at[2 * down(k) + c]
        sized(wfull.at[dpi, y, zp], wx_s.at[k - 1], wx_r.at[k - 1, 0]).wait_send()
        for o in range(1, n_y):
            sized(mine.at[y, zp], wy_s.at[k - 1, o - 1], wy_r.at[k - 1, 0, o - 1]).wait_send()
        sized(mine.at[:, zp], wz_s.at[k - 1], wz_r.at[k - 1, 0, 0]).wait_send()
        sized(mine, wfw_s.at[k - 1], wfw_r.at[k - 1]).wait_send()
        sized(rx.at[k - 1], xs_s.at[k - 1], xs_r.at[k - 1, 0, 0]).wait_send()
    for k in range(pairs):
        sized(rcore.at[k], core_s.at[k], core_r.at[k, 0]).wait_send()
    for o in range(1, n_y):
        sized(ry.at[:, o - 1], yr_s.at[o - 1], yr_r.at[0, o - 1, 0]).wait_send()
        sized(ry.at[:, o - 1], ya_s.at[o - 1], ya_r.at[0, o - 1]).wait_send()
    sized(rz, zr_s, zr_r.at[0, 0]).wait_send()
    sized(rz, za_s, za_r.at[0, 0]).wait_send()
    sized(acore, sa_s, sa_r.at[0]).wait_send()
    for chunk in range(n_dp):
        if full:
            all_s1(chunk).wait_send()
        else:
            for o in range(1, n_pl):
                owner((plane + o) % n_pl, lambda o=o: t_s1(chunk, o).wait_send())
        owner(plane, lambda: all_s2(chunk).wait_send())
    for j in range(2):
        owner(plane, lambda: all_s3(j).wait_send())
        owner(plane, lambda: [t_s4(j, o).wait_send() for o in range(1, n_pl)] and None) if not full else all_s4(j).wait_send()
        t_sd(j).wait_send()


def finish(dims, gu_ref, gv_ref, dw_ref, sm_ref, gu_hbm, gv_hbm, dw_hbm, gw_hbm, bias_ref, gain_ref, shift_ref, dw_f, gw_f, sem, dw_sem):
    gpc, span, chans, width, n_sp, groups, prow = dims
    copies = [
        pltpu.make_async_copy(gu_ref, gu_hbm.at[0], sem.at[0]),
        pltpu.make_async_copy(gv_ref, gv_hbm.at[0], sem.at[1]),
    ]
    for copy in copies:
        copy.start()
    for q in range(gpc):
        for j in range(n_sp):
            dw_f[q * span : (q + 1) * span, j * width : (j + 1) * width] = dw_ref[q, j].astype(F32)
        at = pl.ds(q * span, span)
        copy = pltpu.make_async_copy(dw_f.at[at], dw_hbm.at[at], dw_sem.at[q])
        copy.start()
        copies.append(copy)
    r = lax.broadcasted_iota(jnp.int32, (prow, chans), 0)
    l = lax.broadcasted_iota(jnp.int32, (prow, chans), 1)
    per = span // prow
    hq = gpc // 2
    for g in range(groups):
        chunk, q = divmod(g, gpc)
        xx, j = divmod(chunk, 2)
        for p in range(per):
            block = sm_ref[j, q // hq, q % hq * per + p, xx].astype(F32)
            gw_f[g, p * prow : (p + 1) * prow, :] = jnp.where(r + p * prow >= l, block, 0.0)
            if p == 0:
                turned = pltpu.roll(block[:8], chans // 2, 1)
                for n, ref in enumerate((bias_ref, gain_ref, shift_ref)):
                    ref[g : g + 1, :] = jnp.where(l[:1] < chans // 2, turned[n : n + 1], block[n + 3 : n + 4])
    copy = pltpu.make_async_copy(gw_f, gw_hbm, sem.at[2])
    copy.start()
    copies.append(copy)
    for copy in copies:
        copy.wait()


def on_device(n_sp, n_dp, u_pre, v_pre, d_out, w_mix, mix_bias, norm_gain, norm_shift, w_out):
    _, rows, wide = u_pre.shape
    depth = d_out.shape[2]
    groups, span = w_mix.shape[:2]
    chans = wide // groups
    gpc = groups // n_dp
    width = depth // n_sp
    shard = w_out.shape[0]
    pairs = n_dp // 2
    n_chips = n_sp * pairs
    half_rows = gpc // 2 * span
    prow = max(16, half_rows // n_chips)
    n_own = half_rows // prow
    n_y = 1
    while 4 * n_y * n_y <= n_sp:
        n_y *= 2
    n_z = n_sp // n_y
    dims = (n_y, n_z, n_dp, gpc, span, chans, width, rows, prow, n_own)
    dma = pltpu.SemaphoreType.DMA
    vm = pltpu.VMEM
    piece = (n_y, n_z, span, width)
    w_piece = (n_y, 2, 2, shard // (4 * n_y), depth)
    scratch = [
        vm((rows, wide), BF16), vm((rows, wide), BF16), vm((rows, depth), BF16),
        vm((groups, span, span), BF16),
        vm((groups, 1, span), F32), vm((groups, 1, chans), F32), vm((groups, 1, chans), F32),
        vm((groups, span, chans), F32),
        dma((pairs,)), dma((pairs,)), dma((6,)),
        vm((n_dp,) + w_piece, BF16),
        vm((groups,) + piece, BF16),
        vm((pairs, gpc) + piece, BF16),
        vm((pairs - 1, gpc) + piece, BF16),
        vm((gpc, n_y - 1) + piece[1:], BF16),
        vm((gpc, n_z - 1) + piece[2:], BF16),
        vm((gpc,) + piece, BF16),
        vm((2, rows, 2 * chans), BF16),
        vm((2, 2 * chans, rows), BF16),
        vm((2, span, span), BF16),
        vm((2, span, span), BF16),
        vm((2, 4, span, chans), F32),
        vm((n_dp, 2, n_own, prow, chans), BF16),
        vm((n_dp, n_own, prow, chans), BF16),
        vm((n_dp, n_y * pairs - 1, n_z, prow, chans), BF16),
        vm((n_dp, n_z - 1, prow, chans), BF16),
        vm((2, 2, n_own, pairs, prow, chans), BF16),
        dma, dma,
        dma((pairs - 1,)), dma((pairs - 1, 2)),
        dma((pairs - 1, n_y - 1)), dma((pairs - 1, 2, n_y - 1)),
        dma((pairs - 1,)), dma((pairs - 1, 2, n_y)),
        dma((pairs - 1,)), dma((pairs - 1,)),
        dma((pairs,)), dma((pairs, gpc)),
        dma((pairs - 1,)), dma((pairs - 1, gpc + 1, n_y)),
        dma((n_y - 1,)), dma((gpc + 1, n_y - 1, n_z)),
        dma, dma((gpc + 1, n_z - 1)),
        dma, dma((gpc + 1, n_z - 1)),
        dma((n_y - 1,)), dma((gpc + 1, n_y - 1)),
        dma, dma((n_dp,)),
        dma((n_dp,)), dma((n_dp,)),
        dma((n_dp,)), dma((n_dp,)),
        dma((2,)), dma((2,)),
        dma((2,)), dma((2,)),
        dma((2,)), dma((2,)),
    ]
    spec = pl.BlockSpec(memory_space=pltpu.VMEM)
    hbm = pl.BlockSpec(memory_space=pl.ANY)
    results = pl.pallas_call(
        functools.partial(kernel, dims),
        out_shape=(
            vm((rows, wide), BF16),
            vm((rows, wide), BF16),
            vm((gpc, n_sp, span, width), BF16),
            vm((2, 2, n_own, pairs, prow, chans), BF16),
        ),
        in_specs=[hbm] * 8,
        out_specs=(spec,) * 4,
        scratch_shapes=scratch,
        compiler_params=pltpu.CompilerParams(
            collective_id=0, has_side_effects=True, vmem_limit_bytes=48 * 1024 * 1024,
        ),
    )(
        u_pre[0], v_pre[0], d_out[0], w_mix,
        mix_bias[:, None, :], norm_gain[:, None, :], norm_shift[:, None, :],
        w_out.reshape(w_piece),
    )
    return pl.pallas_call(
        functools.partial(finish, (gpc, span, chans, width, n_sp, groups, prow)),
        out_shape=(
            jax.ShapeDtypeStruct((1, rows, wide), BF16),
            jax.ShapeDtypeStruct((1, rows, wide), BF16),
            jax.ShapeDtypeStruct((shard, depth), F32),
            jax.ShapeDtypeStruct((groups, span, span), F32),
            jax.ShapeDtypeStruct((groups, span), F32),
            jax.ShapeDtypeStruct((groups, chans), F32),
            jax.ShapeDtypeStruct((groups, chans), F32),
        ),
        in_specs=[spec] * 4,
        out_specs=(hbm,) * 4 + (spec,) * 3,
        scratch_shapes=[
            vm((shard, depth), F32), vm((groups, span, span), F32), dma((3,)), dma((gpc,)),
        ],
        compiler_params=pltpu.CompilerParams(vmem_limit_bytes=32 * 1024 * 1024),
    )(*[pltpu.with_memory_space_constraint(r, pltpu.VMEM) for r in results])


def solution(mesh):
    body = functools.partial(on_device, mesh.shape["sp"], mesh.shape["dp"])
    return jax.shard_map(
        body,
        mesh=mesh,
        in_specs=(
            P("dp", "sp", None),
            P("dp", "sp", None),
            P("dp", "sp", None),
            P(),
            P(),
            P(),
            P(),
            P("dp", None),
        ),
        out_specs=(P("dp", "sp", None), P("dp", "sp", None), P("dp", None), P(), P(), P(), P()),
        check_vma=False,
    )
```
